32 devices in a mesh: sp: 8 (over z, x), dp: 4 (over y, core).
Axes of the slice: x: 2, y: 2, z: 4, core: 2. Of those that a mesh axis runs over, the one named last changes fastest.
Arguments:
- queries: bfloat16 [4, 1024, 16, 128], P('dp', 'sp'), may hold values from -6 to 6
- key_rows: bfloat16 [4, 1024, 4, 128], P('dp', 'sp'), may hold values from -6 to 6
- values: bfloat16 [4, 1024, 4, 128], P('dp', 'sp'), may hold values from -6 to 6
- query_gain: float32 [128], replicated, may hold values from 0.4 to 5
- key_gain: float32 [128], replicated, may hold values from 0.4 to 5
- out_weight: bfloat16 [2048, 2048], P('sp', 'dp'), may hold values from -0.125 to 0.125
- residual: bfloat16 [4, 1024, 2048], P('dp', 'sp'), may hold values from -6 to 6
- norm_gain: float32 [2048], replicated, may hold values from 0.1 to 1.9
- expert_gate: bfloat16 [8, 2048, 1792], P('sp'), may hold values from -0.125 to 0.125
- expert_up: bfloat16 [8, 2048, 1792], P('sp'), may hold values from -0.125 to 0.125
- expert_down: bfloat16 [8, 1792, 2048], P('sp'), may hold values from -0.125 to 0.125
- routes: int32 [4, 1024, 2], P('dp', 'sp'), may hold values from 0 to 7, all different within a row; in each aligned block of 64 rows (0 to 63, 64 to 127, ..., all dimensions but the last counted through in order) at most 32 rows name the same one
- route_weight: float32 [4, 1024, 2], P('dp', 'sp'), may hold values from 0.25 to 1
Outputs:
- layer_out: bfloat16 [4, 1024, 2048], P('dp', 'sp')
The draws below stay inside these ranges and needn't reach their ends.
Inputs may be any that keep to these rules, and one draw needn't show every extreme that they name: `routes`: in each aligned block of 64 rows of one device, no expert is named by more than 32 entries, a bound that some block reaches; the two experts of a row differ.
All inputs are finite; a program needn't handle non-finite values.
Results may differ from the reference program's by a relative error of at most 0.0095.
The reference program's roundings to bfloat16 on the way count: a program that leaves them out, or rounds other values in their place, can miss the bound.
Values may be sent and summed in bfloat16 or wider, within the bound.
No kernel may reach another device: no remote copies, remote signals or barrier semaphores. Data moves between devices by JAX's collectives and lax.ppermute only.
A program may use at most 128 MiB of HBM per device.

```python
import math
import jax
import jax.numpy as jnp
import numpy as np
from jax import lax

D = 2048
HEADS = 16
KV_HEADS = 4
HEAD_DIM = 128
EXPERT_FF = 1792
GRID_W = 64
SEQS = 4
LENGTH = 1024
EXPERTS = 8
HALF = 64
CAP = 32


def shared_keys(key):
    drawn = jax.random.normal(jax.random.fold_in(key, 11), (SEQS, LENGTH, KV_HEADS, HEAD_DIM), jnp.float32)
    return jnp.clip(drawn, -6.0, 6.0)


def draw_key_rows(key, part):
    return shared_keys(key).astype(jnp.bfloat16)


def draw_queries(key, part):
    drawn = jax.random.normal(jax.random.fold_in(key, 12), (SEQS, LENGTH, HEADS, HEAD_DIM), jnp.float32)
    drawn = jnp.clip(drawn, -6.0, 6.0)
    return drawn.astype(jnp.bfloat16)


def gain_draw(key, salt):
    drawn = jax.random.normal(jax.random.fold_in(key, salt), (HEAD_DIM,), jnp.float32)
    return 1.0 + 0.18 * jnp.clip(drawn, -3.0, 3.0)


def draw_query_gain(key, part):
    return gain_draw(key, 21)


def draw_key_gain(key, part):
    return gain_draw(key, 22)


def block_levels(stream_key, extent, pieces, low, top_value):
    def one(dim, parts):
        heights = jax.random.uniform(jax.random.fold_in(jax.random.fold_in(stream_key, 6), dim), (parts,), jnp.float32, low / len(pieces), top_value / len(pieces))
        return jnp.repeat(jnp.exp(heights), extent[dim] // parts).reshape((-1,) + (1,) * (len(extent) - dim - 1))

    level = one(*pieces[0])
    for cut in pieces[1:]:
        level = level * one(*cut)
    return level


def shared_out(rng, own, number, rows, number_of, top, reach, skew):
    sequence = jax.random.permutation(rng, number_of)
    packed, ordinary = portions_of(number_of, rows * top, reach, skew, True), portions_of(number_of, rows * top, reach, skew, False)
    places = jnp.arange(number_of)

    def named(tallies, rotation):
        used = int((tallies > 0).sum())
        fixed = max(1, used // 4)
        passed = fixed + (places - fixed + rotation * (used - fixed)) % max(1, number_of - fixed)
        return jnp.zeros((number_of,), jnp.int32).at[sequence[jnp.where(places < fixed, places, passed)]].set(jnp.asarray(tallies, jnp.int32))

    tallies = jnp.where(number % 4 == 0, named(packed, number // 4), named(ordinary, number - number // 4 - 1))
    mixed = jax.random.permutation(jax.random.fold_in(own, 3), number_of)
    donor, sink = mixed[0:number_of // 2 * 2:2], mixed[1:number_of // 2 * 2:2]
    margin = jnp.minimum(tallies[donor] - 1, reach - tallies[sink]) // 2
    margin = jnp.where((donor == sequence[0]) | (sink == sequence[0]) | (tallies[sink] == 0), 0, jnp.maximum(margin, 0))
    passed = jax.random.randint(jax.random.fold_in(own, 4), (number_of // 2,), 0, 1 << 20) % (margin + 1)
    tallies = tallies.at[donor].add(-passed).at[sink].add(passed)
    items = jnp.searchsorted(jnp.cumsum(tallies), jnp.arange(rows * top), side="right").astype(jnp.int32)
    listing = items.reshape(top, rows).T
    listing = listing[jax.random.permutation(jax.random.fold_in(own, 1), rows)]
    rotation = jax.random.randint(jax.random.fold_in(own, 2), (rows, 1), 0, top)
    return jnp.take_along_axis(listing, (jnp.arange(top)[None, :] + rotation) % top, axis=1)


def portions_of(amount, total, most, slope, full):
    weights = [(1 << 20) // math.isqrt(grade ** slope) + 1 for grade in range(1, amount + 1)]
    largest = most if full else min(most, max(-(-total // amount), total * weights[0] // sum(weights)))
    least = 1 if total - largest >= amount - 1 else 0
    counts, spare = [largest] + [least] * (amount - 1), total - largest - least * (amount - 1)
    while spare > 0:
        movable = [i for i in range(1, amount) if counts[i] < largest] or [i for i in range(1, amount) if counts[i] < most]
        mass, budget = sum([weights[i] for i in movable]), spare
        for i in movable:
            addition = min(most - counts[i], max(1, budget * weights[i] // mass), spare)
            counts[i] = counts[i] + addition
            spare = spare - addition
    return np.array(counts)


def gaussian(own_key, dims, deviation, bound, pieces=(), kind=jnp.bfloat16):
    array = jax.random.normal(own_key, dims, jnp.float32) * deviation
    if len(pieces) > 0:
        array = block_levels(own_key, dims, pieces, -0.22, 0.18) * array
    return jnp.clip(array, min=-bound, max=bound).astype(kind)


def setup_inputs(seed: int = 0) -> dict:
    streams_of = jax.random.split(jax.random.key(seed), 14)
    queries = draw_queries(jax.random.fold_in(streams_of[13], 71), 0)
    key_rows = draw_key_rows(jax.random.fold_in(streams_of[13], 71), 0)
    values = gaussian(streams_of[2], (SEQS, LENGTH, KV_HEADS, HEAD_DIM), 1.0, 6.0, ((0, 4), (1, 8)))
    query_gain = draw_query_gain(jax.random.fold_in(streams_of[13], 71), 0)
    key_gain = draw_key_gain(jax.random.fold_in(streams_of[13], 71), 0)
    out_weight = gaussian(streams_of[5], (HEADS * HEAD_DIM, D), (HEADS * HEAD_DIM) ** -0.5, 0.125, ((0, 8), (1, 4)))
    residual = gaussian(streams_of[6], (SEQS, LENGTH, D), 1.0, 6.0, ((0, 4), (1, 8)))
    norm_gain = jnp.clip(1.0 + 0.18 * jax.random.normal(streams_of[7], (D,), jnp.float32), 0.1, 1.9)
    expert_gate = gaussian(streams_of[8], (EXPERTS, D, EXPERT_FF), D ** -0.5, 0.125, ((0, 8),))
    expert_up = gaussian(streams_of[9], (EXPERTS, D, EXPERT_FF), D ** -0.5, 0.125, ((0, 8),))
    expert_down = gaussian(streams_of[10], (EXPERTS, EXPERT_FF, D), EXPERT_FF ** -0.5, 0.125, ((0, 8),))
    routes_keys = jax.random.split(jax.random.fold_in(streams_of[11], 1), SEQS * LENGTH // HALF)
    routes_turns = jax.random.permutation(jax.random.fold_in(streams_of[11], 3), SEQS * LENGTH // HALF)
    routes = jax.vmap(lambda own, number: shared_out(jax.random.fold_in(streams_of[11], 2), own, number, HALF, EXPERTS, 2, CAP, 2))(routes_keys, routes_turns).reshape((SEQS, LENGTH, 2))
    route_weight = jnp.clip(0.25 + 0.75 * jax.random.uniform(streams_of[12], (SEQS, LENGTH, 2), jnp.float32) ** block_levels(streams_of[12], (SEQS, LENGTH, 2), ((0, 4), (1, 8)), -0.2, 0.2), 0.25, 1.0)
    return {"queries": queries, "key_rows": key_rows, "values": values, "query_gain": query_gain, "key_gain": key_gain, "out_weight": out_weight, "residual": residual, "norm_gain": norm_gain, "expert_gate": expert_gate, "expert_up": expert_up, "expert_down": expert_down, "routes": routes, "route_weight": route_weight}


EPS = 1e-06
THETA = 10000.0

def rotate_half(vector, position):
    half_size = vector.shape[-1] // 2
    inverse = THETA ** (-jnp.arange(half_size, dtype=jnp.float32) / half_size)
    angles = position[:, None] * inverse[None, :]
    cosine = jnp.cos(angles)[:, None, :]
    sine_part = jnp.sin(angles)[:, None, :]
    first_part = vector[..., :half_size]
    second_part = vector[..., half_size:]
    return jnp.concatenate([first_part * cosine - second_part * sine_part, first_part * sine_part + second_part * cosine], axis=-1)

def normalize_rotate(vector, gain, positions):
    as_float = vector.astype(jnp.float32)
    scaled = as_float * lax.rsqrt(lax.optimization_barrier(jnp.mean(as_float * as_float, axis=-1, keepdims=True)) + EPS) * gain
    grid_row = (positions // GRID_W).astype(jnp.float32)
    column = (positions % GRID_W).astype(jnp.float32)
    quarter = scaled.shape[-1] // 2
    turned = jnp.concatenate([rotate_half(scaled[..., :quarter], grid_row), rotate_half(scaled[..., quarter:], column)], axis=-1)
    return turned.astype(jnp.bfloat16)

def softmax_rows(scores):
    row_max = lax.optimization_barrier(jnp.max(scores, axis=-1, keepdims=True))
    exponent = jnp.exp(scores - row_max)
    return (exponent / lax.optimization_barrier(jnp.sum(exponent, axis=-1, keepdims=True))).astype(jnp.bfloat16)

def attend_sequence(rot_query, rot_key, value_rows):
    length = rot_query.shape[0]
    group_size = HEADS // KV_HEADS
    block_size = min(512, length)
    key_float = rot_key.astype(jnp.float32)
    value_float = value_rows.astype(jnp.float32)
    grouped = rot_query.reshape(length // block_size, block_size, KV_HEADS, group_size, HEAD_DIM)

    def one_block(query_block):
        scores = jnp.einsum('qhgd,khd->hgqk', query_block.astype(jnp.float32), key_float) * HEAD_DIM ** (-0.5)
        weights = softmax_rows(scores)
        return jnp.einsum('hgqk,khd->qhgd', weights.astype(jnp.float32), value_float).astype(jnp.bfloat16)
    outputs = lax.map(one_block, grouped)
    return outputs.reshape(length, HEADS * HEAD_DIM)

def reference(queries, key_rows, values, query_gain, key_gain, out_weight, residual, norm_gain, expert_gate, expert_up, expert_down, routes, route_weight):
    positions = jnp.arange(LENGTH, dtype=jnp.int32)

    def one_sequence(inputs):
        query_seq, key_seq, value_seq, residual_seq = inputs
        rot_query = normalize_rotate(query_seq, query_gain, positions)
        rot_key = normalize_rotate(key_seq, key_gain, positions)
        attended = attend_sequence(rot_query, rot_key, value_seq)
        return residual_seq.astype(jnp.float32) + jnp.dot(attended, out_weight, preferred_element_type=jnp.float32)
    mixed_sum = lax.map(one_sequence, (queries, key_rows, values, residual))
    flat_mixed = mixed_sum.reshape(-1, D)
    normed = (flat_mixed * lax.rsqrt(lax.optimization_barrier(jnp.mean(flat_mixed * flat_mixed, axis=-1, keepdims=True)) + EPS) * norm_gain).astype(jnp.bfloat16)
    tokens = flat_mixed.shape[0]
    blocks = tokens // HALF
    chosen = routes.reshape(blocks, HALF * 2)
    onehot = (chosen[..., None] == jnp.arange(EXPERTS, dtype=jnp.int32)).astype(jnp.int32)
    slot_rank = lax.optimization_barrier(jnp.sum(jnp.cumsum(onehot, axis=1) * onehot, axis=-1)) - 1
    slot_index = jnp.arange(blocks, dtype=jnp.int32)[:, None] * CAP + slot_rank
    per_expert = blocks * CAP
    target = (chosen * per_expert + slot_index).reshape(-1).astype(jnp.int32)
    source_row = jnp.repeat(jnp.arange(tokens, dtype=jnp.int32), 2)
    row_table = jnp.full((EXPERTS * per_expert,), tokens, jnp.int32).at[target].set(source_row)
    padded = jnp.concatenate([normed, jnp.zeros((1, D), jnp.bfloat16)], axis=0)

    def one_expert(inputs):
        row_ids, gate_weight, up_weight, down_weight = inputs
        selected = padded[row_ids]
        gate_part = jnp.dot(selected, gate_weight, preferred_element_type=jnp.float32)
        up_part = jnp.dot(selected, up_weight, preferred_element_type=jnp.float32)
        hidden = (jax.nn.silu(gate_part) * up_part).astype(jnp.bfloat16)
        return jnp.dot(hidden, down_weight, preferred_element_type=jnp.float32).astype(jnp.bfloat16)
    outputs = lax.map(one_expert, (row_table.reshape(EXPERTS, per_expert), expert_gate, expert_up, expert_down))
    picked = outputs.reshape(-1, D)[target].astype(jnp.float32).reshape(tokens, 2, D)
    weights = route_weight.reshape(tokens, 2, 1)
    result = flat_mixed + lax.optimization_barrier(jnp.sum(picked * weights, axis=1))
    return result.reshape(SEQS, LENGTH, D).astype(jnp.bfloat16)
```

```python
import jax
import jax.numpy as jnp
from jax import lax
from jax.experimental import pallas as pl
from jax.experimental.pallas import tpu as pltpu
from jax.sharding import PartitionSpec as P

GRID_W = 64
EPS = 1e-06
THETA = 10000.0
F32 = jnp.float32
BF16 = jnp.bfloat16


def swap(array, axis, bits):
    size = lax.axis_size(axis)
    return lax.ppermute(array, axis, [(i, i ^ bits) for i in range(size)])


def angle_tables(positions, width):
    lane = jnp.arange(width, dtype=jnp.int32)
    half = width // 2
    quarter = half // 2
    inverse = THETA ** (-(lane % quarter).astype(F32) / quarter)
    place = jnp.where(
        lane[None, :] < half, (positions // GRID_W)[:, None], (positions % GRID_W)[:, None]
    ).astype(F32)
    angles = place * inverse[None, :]
    sign = jnp.where((lane % half) < quarter, -1.0, 1.0)
    return jnp.cos(angles), jnp.sin(angles) * sign[None, :]


def pack_rows(queries, keys, values, query_gain, key_gain, cosine, sine, parts):
    rows, query_width = queries.shape
    width = cosine.shape[1]
    heads = query_width // width
    kv_heads = keys.shape[1] // width
    group = heads // kv_heads
    per = heads // parts
    kv_per = max(1, per // group)
    block = (per + 2 * kv_per) * width

    def body(q_ref, k_ref, v_ref, qg_ref, kg_ref, c_ref, s_ref, o_ref):
        lane = lax.broadcasted_iota(jnp.int32, (rows, width), 1)
        low = (lane % (width // 2)) < (width // 4)
        cos = c_ref[...]
        sin = s_ref[...]

        def turned(part, gain):
            x = part.astype(F32)
            a = x * lax.rsqrt(jnp.mean(x * x, axis=-1, keepdims=True) + EPS) * gain
            other = jnp.where(
                low, pltpu.roll(a, width - width // 4, 1), pltpu.roll(a, width // 4, 1)
            )
            return (a * cos + other * sin).astype(BF16)

        for head in range(heads):
            at = (head % per) * width
            o_ref[head // per, :, at : at + width] = turned(
                q_ref[:, head * width : (head + 1) * width], qg_ref[...]
            )
        turned_keys = [
            turned(k_ref[:, h * width : (h + 1) * width], kg_ref[...]) for h in range(kv_heads)
        ]
        for part in range(parts):
            for i in range(kv_per):
                h = (part * per) // group + i
                at = (per + i) * width
                o_ref[part, :, at : at + width] = turned_keys[h]
                at = (per + kv_per + i) * width
                o_ref[part, :, at : at + width] = v_ref[:, h * width : (h + 1) * width]

    return pl.pallas_call(
        body, out_shape=jax.ShapeDtypeStruct((parts, rows, block), BF16), name="pack_rows"
    )(queries, keys, values, query_gain[None], key_gain[None], cosine, sine)


def attend(packed, per, kv_per, width):
    length, full = packed.shape
    rows = min(256, length)

    def body(q_ref, all_ref, o_ref):
        for head in range(per):
            kv = head * kv_per // per
            q = q_ref[:, head * width : (head + 1) * width]
            k = all_ref[:, (per + kv) * width : (per + kv + 1) * width]
            v = all_ref[:, (per + kv_per + kv) * width : (per + kv_per + kv + 1) * width]
            scores = lax.dot_general(
                q, k, (((1,), (1,)), ((), ())), preferred_element_type=F32
            ) * width ** (-0.5)
            e = jnp.exp(scores - jnp.max(scores, axis=-1, keepdims=True))
            weights = (e * (1.0 / jnp.sum(e, axis=-1, keepdims=True))).astype(BF16)
            o_ref[:, head * width : (head + 1) * width] = jnp.dot(
                weights, v, preferred_element_type=F32
            ).astype(BF16)

    return pl.pallas_call(
        body,
        grid=(length // rows,),
        in_specs=[
            pl.BlockSpec((rows, full), lambda i: (i, 0)),
            pl.BlockSpec((length, full), lambda i: (0, 0)),
        ],
        out_specs=pl.BlockSpec((rows, per * width), lambda i: (i, 0)),
        out_shape=jax.ShapeDtypeStruct((length, per * width), BF16),
        name="attend",
    )(packed, packed)


def expert_rows(blocks, gate, up, down):
    count = len(blocks)
    rows, model = blocks[0].shape
    hidden_width = gate.shape[1]
    tile = 256
    steps = hidden_width // tile

    def body(*refs):
        x_refs = refs[:count]
        g_ref, u_ref, d_ref = refs[count : count + 3]
        o_refs = refs[count + 3 : 2 * count + 3]
        x_all, acc = refs[2 * count + 3 :]
        step = pl.program_id(0)

        @pl.when(step == 0)
        def _():
            for i in range(count):
                x_all[i * rows : (i + 1) * rows, :] = x_refs[i][...]

        x = x_all[...]
        g = jnp.dot(x, g_ref[...], preferred_element_type=F32)
        u = jnp.dot(x, u_ref[...], preferred_element_type=F32)
        hidden = (g / (1.0 + jnp.exp(-g)) * u).astype(BF16)
        y = jnp.dot(hidden, d_ref[...], preferred_element_type=F32)

        @pl.when(step == 0)
        def _():
            acc[...] = y

        @pl.when(step > 0)
        def _():
            acc[...] += y

        @pl.when(step == steps - 1)
        def _():
            for i in range(count):
                o_refs[i][...] = acc[i * rows : (i + 1) * rows, :].astype(BF16)

    whole = pl.BlockSpec((rows, model), lambda i: (0, 0))
    return pl.pallas_call(
        body,
        grid=(steps,),
        in_specs=[whole] * count
        + [
            pl.BlockSpec((model, tile), lambda i: (0, i)),
            pl.BlockSpec((model, tile), lambda i: (0, i)),
            pl.BlockSpec((tile, model), lambda i: (i, 0)),
        ],
        out_specs=[whole] * count,
        out_shape=[jax.ShapeDtypeStruct((rows, model), BF16)] * count,
        scratch_shapes=[
            pltpu.VMEM((count * rows, model), BF16),
            pltpu.VMEM((count * rows, model), F32),
        ],
        name="expert_rows",
    )(*blocks, gate, up, down)


def slots_of(chosen, capacity, experts):
    tokens = chosen.shape[0]
    by_block = chosen.reshape(2, tokens)
    onehot = (by_block[..., None] == jnp.arange(experts, dtype=jnp.int32)).astype(F32)
    earlier = (jnp.arange(tokens)[:, None] > jnp.arange(tokens)[None, :]).astype(F32)
    before = jnp.einsum("ij,bje->bie", earlier, onehot, preferred_element_type=F32)
    rank = jnp.sum(before * onehot, axis=-1).astype(jnp.int32)
    return (jnp.arange(2, dtype=jnp.int32)[:, None] * capacity + rank).reshape(tokens, 2)


def on_device(
    queries, key_rows, values, query_gain, key_gain, out_weight, residual, norm_gain,
    expert_gate, expert_up, expert_down, routes, route_weight,
):
    parts = lax.axis_size("sp")
    columns = lax.axis_size("dp")
    me = lax.axis_index("sp")
    _, tokens, heads, width = queries.shape
    kv_heads = key_rows.shape[2]
    group = heads // kv_heads
    per = heads // parts
    kv_per = max(1, per // group)
    model = residual.shape[-1]
    half = parts // 2
    near = parts // 4

    positions = me * tokens + jnp.arange(tokens, dtype=jnp.int32)
    cosine, sine = angle_tables(positions, width)
    packed = pack_rows(
        queries.reshape(tokens, heads * width),
        key_rows.reshape(tokens, kv_heads * width),
        values.reshape(tokens, kv_heads * width),
        query_gain, key_gain, cosine, sine, parts,
    )
    by_head = lax.all_to_all(packed, "sp", split_axis=0, concat_axis=0, tiled=True)

    shards = [None] * parts
    for far in range(4):
        shard = out_weight if far == 0 else swap(out_weight, "sp", far * near)
        shards[far * near] = shard
        for close in range(1, near):
            shards[far * near + close] = swap(shard, "sp", close)
    own_columns = jnp.concatenate(shards, axis=0)
    core_columns = swap(own_columns, "dp", 1)

    experts = expert_gate.shape[0] * parts
    capacity = max(2, 4 * (tokens // 2) // experts)
    slots = 2 * capacity
    chosen = routes[0]
    slot = slots_of(chosen, capacity, experts)
    weight = route_weight[0]
    chosen_far = swap(chosen, "sp", half)
    slot_far = swap(slot, "sp", half)
    weight_far = swap(weight, "sp", half)
    place = jnp.arange(half * slots, dtype=jnp.int32)
    place_expert = me ^ (place // slots)
    place_slot = place % slots

    def selection(chosen, slot):
        return [
            (chosen[:, j, None] == place_expert[None]) & (slot[:, j, None] == place_slot[None])
            for j in range(2)
        ]

    pick = selection(chosen, slot)
    pick_far = selection(chosen_far, slot_far)

    attended = attend(by_head.reshape(parts * tokens, -1), per, kv_per, width)
    returned = lax.all_to_all(
        attended.reshape(parts, tokens, per * width), "sp", split_axis=0, concat_axis=0, tiled=True
    )
    rows = jnp.concatenate(
        [lax.dynamic_index_in_dim(returned, me ^ k, 0, keepdims=False) for k in range(parts)],
        axis=1,
    )

    chips = columns // 2
    gathered = jnp.concatenate([rows] + [swap(rows, "dp", 2 * k) for k in range(1, chips)], axis=0)
    mine = jnp.dot(gathered, own_columns, preferred_element_type=F32).astype(BF16)
    other = jnp.dot(gathered, core_columns, preferred_element_type=F32).astype(BF16)
    first = lax.axis_index("dp") % 2 == 0
    both = jnp.concatenate(
        [jnp.where(first, mine, other), jnp.where(first, other, mine)], axis=1
    ).reshape(chips, tokens, -1)
    back = [both[0]] + [swap(both[k], "dp", 2 * k) for k in range(1, chips)]
    chip = lax.axis_index("dp") // 2
    if chips == 2:
        ordered = [jnp.where(chip == 0, back[0], back[1]), jnp.where(chip == 0, back[1], back[0])]
    else:
        stacked = jnp.stack(back)
        ordered = [
            lax.dynamic_index_in_dim(stacked, chip ^ k, 0, keepdims=False) for k in range(chips)
        ]
    projected = jnp.concatenate(ordered, axis=1).astype(F32)
    mixed_sum = residual[0].astype(F32) + projected
    normed = (
        mixed_sum
        * lax.rsqrt(jnp.mean(mixed_sum * mixed_sum, axis=-1, keepdims=True) + EPS)
        * norm_gain
    ).astype(BF16)

    normed_far = swap(normed, "sp", half)

    def serve(source, picks):
        chosen_rows = (picks[0] | picks[1]).astype(BF16)
        sent = lax.dot_general(
            chosen_rows, source, (((0,), (0,)), ((), ())), preferred_element_type=F32
        ).astype(BF16)
        blocks = [sent[k * slots : (k + 1) * slots] for k in range(half)]
        blocks = [blocks[0]] + [swap(blocks[k], "sp", k) for k in range(1, half)]
        results = expert_rows(blocks, expert_gate[0], expert_up[0], expert_down[0])
        return [results[0]] + [swap(results[k], "sp", k) for k in range(1, half)]

    def combine(results, picks, weight):
        flat = jnp.concatenate(results, axis=0)
        return sum(
            jnp.dot(picks[j].astype(BF16), flat, preferred_element_type=F32) * weight[:, j, None]
            for j in range(2)
        )

    near_results = serve(normed, pick)
    far_results = serve(normed_far, pick_far)
    crossed = swap(combine(far_results, pick_far, weight_far).astype(BF16), "sp", half)
    result = mixed_sum + combine(near_results, pick, weight) + crossed.astype(F32)
    return result.astype(BF16)[None]


def solution(mesh):
    in_specs = (
        P("dp", "sp", None, None),
        P("dp", "sp", None, None),
        P("dp", "sp", None, None),
        P(),
        P(),
        P("sp", "dp"),
        P("dp", "sp", None),
        P(),
        P("sp", None, None),
        P("sp", None, None),
        P("sp", None, None),
        P("dp", "sp", None),
        P("dp", "sp", None),
    )
    out_specs = P("dp", "sp", None)
    return jax.shard_map(
        on_device, mesh=mesh, in_specs=in_specs, out_specs=out_specs, check_vma=False
    )
```

```python
import jax
import jax.numpy as jnp
from jax import lax
from jax.experimental import pallas as pl
from jax.experimental.pallas import tpu as pltpu
from jax.sharding import PartitionSpec as P


GRID_W = 64
EPS = 1e-06
THETA = 10000.0
F32 = jnp.float32
BF16 = jnp.bfloat16


def swap(array, axis, bits):
    size = lax.axis_size(axis)
    return lax.ppermute(array, axis, [(i, i ^ bits) for i in range(size)])


def angle_tables(positions, width):
    lane = jnp.arange(width, dtype=jnp.int32)
    half = width // 2
    quarter = half // 2
    inverse = THETA ** (-(lane % quarter).astype(F32) / quarter)
    place = jnp.where(
        lane[None, :] < half, (positions // GRID_W)[:, None], (positions % GRID_W)[:, None]
    ).astype(F32)
    angles = place * inverse[None, :]
    sign = jnp.where((lane % half) < quarter, -1.0, 1.0)
    return jnp.cos(angles), jnp.sin(angles) * sign[None, :]


def pack_rows(queries, keys, values, query_gain, key_gain, cosine, sine, parts):
    rows, query_width = queries.shape
    width = cosine.shape[1]
    heads = query_width // width
    kv_heads = keys.shape[1] // width
    group = heads // kv_heads
    per = heads // parts
    kv_per = max(1, per // group)
    block = (per + 2 * kv_per) * width

    def body(q_ref, k_ref, v_ref, qg_ref, kg_ref, c_ref, s_ref, o_ref):
        lane = lax.broadcasted_iota(jnp.int32, (rows, width), 1)
        low = (lane % (width // 2)) < (width // 4)
        cos = c_ref[...]
        sin = s_ref[...]

        def turned(part, gain):
            x = part.astype(F32)
            a = x * lax.rsqrt(jnp.mean(x * x, axis=-1, keepdims=True) + EPS) * gain
            other = jnp.where(
                low, pltpu.roll(a, width - width // 4, 1), pltpu.roll(a, width // 4, 1)
            )
            return (a * cos + other * sin).astype(BF16)

        for head in range(heads):
            at = (head % per) * width
            o_ref[head // per, :, at : at + width] = turned(
                q_ref[:, head * width : (head + 1) * width], qg_ref[...]
            )
        turned_keys = [
            turned(k_ref[:, h * width : (h + 1) * width], kg_ref[...]) for h in range(kv_heads)
        ]
        for part in range(parts):
            for i in range(kv_per):
                h = (part * per) // group + i
                at = (per + i) * width
                o_ref[part, :, at : at + width] = turned_keys[h]
                at = (per + kv_per + i) * width
                o_ref[part, :, at : at + width] = v_ref[:, h * width : (h + 1) * width]

    return pl.pallas_call(
        body, out_shape=jax.ShapeDtypeStruct((parts, rows, block), BF16), name="pack_rows"
    )(queries, keys, values, query_gain[None], key_gain[None], cosine, sine)


def attend(packed, per, kv_per, width):
    length, full = packed.shape
    rows = min(256, length)

    def body(q_ref, all_ref, o_ref):
        for head in range(per):
            kv = head * kv_per // per
            q = q_ref[:, head * width : (head + 1) * width]
            k = all_ref[:, (per + kv) * width : (per + kv + 1) * width]
            v = all_ref[:, (per + kv_per + kv) * width : (per + kv_per + kv + 1) * width]
            scores = lax.dot_general(
                q, k, (((1,), (1,)), ((), ())), preferred_element_type=F32
            ) * width ** (-0.5)
            e = jnp.exp(scores - jnp.max(scores, axis=-1, keepdims=True))
            weights = (e * (1.0 / jnp.sum(e, axis=-1, keepdims=True))).astype(BF16)
            o_ref[:, head * width : (head + 1) * width] = jnp.dot(
                weights, v, preferred_element_type=F32
            ).astype(BF16)

    return pl.pallas_call(
        body,
        grid=(length // rows,),
        in_specs=[
            pl.BlockSpec((rows, full), lambda i: (i, 0)),
            pl.BlockSpec((length, full), lambda i: (0, 0)),
        ],
        out_specs=pl.BlockSpec((rows, per * width), lambda i: (i, 0)),
        out_shape=jax.ShapeDtypeStruct((length, per * width), BF16),
        name="attend",
    )(packed, packed)


def expert_rows(blocks, gate, up, down):
    count = len(blocks)
    rows, model = blocks[0].shape
    hidden_width = gate.shape[1]
    tile = 256
    steps = hidden_width // tile

    def body(*refs):
        x_refs = refs[:count]
        g_ref, u_ref, d_ref = refs[count : count + 3]
        o_refs = refs[count + 3 : 2 * count + 3]
        x_all, acc = refs[2 * count + 3 :]
        step = pl.program_id(0)

        @pl.when(step == 0)
        def _():
            for i in range(count):
                x_all[i * rows : (i + 1) * rows, :] = x_refs[i][...]

        x = x_all[...]
        g = jnp.dot(x, g_ref[...], preferred_element_type=F32)
        u = jnp.dot(x, u_ref[...], preferred_element_type=F32)
        hidden = (g / (1.0 + jnp.exp(-g)) * u).astype(BF16)
        y = jnp.dot(hidden, d_ref[...], preferred_element_type=F32)

        @pl.when(step == 0)
        def _():
            acc[...] = y

        @pl.when(step > 0)
        def _():
            acc[...] += y

        @pl.when(step == steps - 1)
        def _():
            for i in range(count):
                o_refs[i][...] = acc[i * rows : (i + 1) * rows, :].astype(BF16)

    whole = pl.BlockSpec((rows, model), lambda i: (0, 0))
    return pl.pallas_call(
        body,
        grid=(steps,),
        in_specs=[whole] * count
        + [
            pl.BlockSpec((model, tile), lambda i: (0, i)),
            pl.BlockSpec((model, tile), lambda i: (0, i)),
            pl.BlockSpec((tile, model), lambda i: (i, 0)),
        ],
        out_specs=[whole] * count,
        out_shape=[jax.ShapeDtypeStruct((rows, model), BF16)] * count,
        scratch_shapes=[
            pltpu.VMEM((count * rows, model), BF16),
            pltpu.VMEM((count * rows, model), F32),
        ],
        name="expert_rows",
    )(*blocks, gate, up, down)


def slots_of(chosen, capacity, experts):
    tokens = chosen.shape[0]
    by_block = chosen.reshape(2, tokens)
    onehot = (by_block[..., None] == jnp.arange(experts, dtype=jnp.int32)).astype(F32)
    earlier = (jnp.arange(tokens)[:, None] > jnp.arange(tokens)[None, :]).astype(F32)
    before = jnp.einsum("ij,bje->bie", earlier, onehot, preferred_element_type=F32)
    rank = jnp.sum(before * onehot, axis=-1).astype(jnp.int32)
    return (jnp.arange(2, dtype=jnp.int32)[:, None] * capacity + rank).reshape(tokens, 2)


def on_device(
    queries, key_rows, values, query_gain, key_gain, out_weight, residual, norm_gain,
    expert_gate, expert_up, expert_down, routes, route_weight,
):
    parts = lax.axis_size("sp")
    columns = lax.axis_size("dp")
    me = lax.axis_index("sp")
    _, tokens, heads, width = queries.shape
    kv_heads = key_rows.shape[2]
    group = heads // kv_heads
    per = heads // parts
    kv_per = max(1, per // group)
    half = parts // 2
    near = parts // 4

    positions = me * tokens + jnp.arange(tokens, dtype=jnp.int32)
    cosine, sine = angle_tables(positions, width)
    packed = pack_rows(
        queries.reshape(tokens, heads * width),
        key_rows.reshape(tokens, kv_heads * width),
        values.reshape(tokens, kv_heads * width),
        query_gain, key_gain, cosine, sine, parts,
    )
    by_head = lax.all_to_all(packed, "sp", split_axis=0, concat_axis=0, tiled=True)

    shards = [None] * 4
    for far in range(4):
        shards[far] = out_weight if far == 0 else swap(out_weight, "sp", far * near)

    experts = expert_gate.shape[0] * parts
    capacity = max(2, 4 * (tokens // 2) // experts)
    slots = 2 * capacity
    chosen = routes[0]
    slot = slots_of(chosen, capacity, experts)
    weight = route_weight[0]
    chosen_far = swap(chosen, "sp", half)
    slot_far = swap(slot, "sp", half)
    weight_far = swap(weight, "sp", half)
    place = jnp.arange(half * slots, dtype=jnp.int32)
    place_expert = me ^ (place // slots)
    place_slot = place % slots

    def selection(chosen, slot):
        return [
            (chosen[:, j, None] == place_expert[None]) & (slot[:, j, None] == place_slot[None])
            for j in range(2)
        ]

    pick = selection(chosen, slot)
    pick_far = selection(chosen_far, slot_far)

    attended = attend(by_head.reshape(parts * tokens, -1), per, kv_per, width)
    attended, shards = lax.optimization_barrier((attended, shards))
    whole = []
    for far in range(4):
        whole.append(shards[far])
        for close in range(1, near):
            whole.append(swap(shards[far], "sp", close))
    own_columns = jnp.concatenate(whole, axis=0)
    core_columns = swap(own_columns, "dp", 1)
    returned = lax.all_to_all(
        attended.reshape(parts, tokens, per * width), "sp", split_axis=0, concat_axis=0, tiled=True
    )
    rows = jnp.concatenate(
        [lax.dynamic_index_in_dim(returned, me ^ k, 0, keepdims=False) for k in range(parts)],
        axis=1,
    )

    chips = columns // 2
    gathered = jnp.concatenate([rows] + [swap(rows, "dp", 2 * k) for k in range(1, chips)], axis=0)
    mine = jnp.dot(gathered, own_columns, preferred_element_type=F32).astype(BF16)
    other = jnp.dot(gathered, core_columns, preferred_element_type=F32).astype(BF16)
    first = lax.axis_index("dp") % 2 == 0
    both = jnp.concatenate(
        [jnp.where(first, mine, other), jnp.where(first, other, mine)], axis=1
    ).reshape(chips, tokens, -1)
    back = [both[0]] + [swap(both[k], "dp", 2 * k) for k in range(1, chips)]
    chip = lax.axis_index("dp") // 2
    if chips == 2:
        ordered = [jnp.where(chip == 0, back[0], back[1]), jnp.where(chip == 0, back[1], back[0])]
    else:
        stacked = jnp.stack(back)
        ordered = [
            lax.dynamic_index_in_dim(stacked, chip ^ k, 0, keepdims=False) for k in range(chips)
        ]
    projected = jnp.concatenate(ordered, axis=1).astype(F32)
    mixed_sum = residual[0].astype(F32) + projected
    normed = (
        mixed_sum
        * lax.rsqrt(jnp.mean(mixed_sum * mixed_sum, axis=-1, keepdims=True) + EPS)
        * norm_gain
    ).astype(BF16)

    normed_far = swap(normed, "sp", half)

    def send(source, picks):
        chosen_rows = (picks[0] | picks[1]).astype(BF16)
        sent = lax.dot_general(
            chosen_rows, source, (((0,), (0,)), ((), ())), preferred_element_type=F32
        ).astype(BF16)
        return exchange([sent[k * slots : (k + 1) * slots] for k in range(half)])

    def exchange(blocks):
        moved = [blocks[0]]
        for k in range(1, half):
            moved.append(swap(blocks[k], "sp", k))
        return moved

    def serve(blocks):
        return expert_rows(blocks, expert_gate[0], expert_up[0], expert_down[0])

    def combine(results, picks, weight):
        flat = jnp.concatenate(results, axis=0)
        return sum(
            jnp.dot(picks[j].astype(BF16), flat, preferred_element_type=F32) * weight[:, j, None]
            for j in range(2)
        )

    near_blocks = send(normed, pick)
    far_blocks = send(normed_far, pick_far)
    near_results = serve(near_blocks)
    far_results = serve(far_blocks)
    near_results = exchange(near_results)
    far_results = exchange(far_results)
    crossed = swap(combine(far_results, pick_far, weight_far).astype(BF16), "sp", half)
    result = mixed_sum + combine(near_results, pick, weight) + crossed.astype(F32)
    return result.astype(BF16)[None]


def solution(mesh):
    in_specs = (
        P("dp", "sp", None, None),
        P("dp", "sp", None, None),
        P("dp", "sp", None, None),
        P(),
        P(),
        P("sp", "dp"),
        P("dp", "sp", None),
        P(),
        P("sp", None, None),
        P("sp", None, None),
        P("sp", None, None),
        P("dp", "sp", None),
        P("dp", "sp", None),
    )
    out_specs = P("dp", "sp", None)

    return jax.shard_map(
        on_device, mesh=mesh, in_specs=in_specs, out_specs=out_specs, check_vma=False
    )
```

```python
import jax
import jax.numpy as jnp
from jax import lax
from jax.experimental import pallas as pl
from jax.experimental.pallas import tpu as pltpu
from jax.sharding import PartitionSpec as P


GRID_W = 64
EPS = 1e-06
THETA = 10000.0
F32 = jnp.float32
BF16 = jnp.bfloat16


def swap(array, axis, bits):
    size = lax.axis_size(axis)
    return lax.ppermute(array, axis, [(i, i ^ bits) for i in range(size)])


def angle_tables(positions, width):
    lane = jnp.arange(width, dtype=jnp.int32)
    half = width // 2
    quarter = half // 2
    inverse = THETA ** (-(lane % quarter).astype(F32) / quarter)
    place = jnp.where(
        lane[None, :] < half, (positions // GRID_W)[:, None], (positions % GRID_W)[:, None]
    ).astype(F32)
    angles = place * inverse[None, :]
    sign = jnp.where((lane % half) < quarter, -1.0, 1.0)
    return jnp.cos(angles), jnp.sin(angles) * sign[None, :]


def pack_rows(queries, keys, values, query_gain, key_gain, cosine, sine, parts):
    rows, query_width = queries.shape
    width = cosine.shape[1]
    heads = query_width // width
    kv_heads = keys.shape[1] // width
    group = heads // kv_heads
    per = heads // parts
    kv_per = max(1, per // group)
    block = (per + 2 * kv_per) * width

    def body(q_ref, k_ref, v_ref, qg_ref, kg_ref, c_ref, s_ref, o_ref):
        lane = lax.broadcasted_iota(jnp.int32, (rows, width), 1)
        low = (lane % (width // 2)) < (width // 4)
        cos = c_ref[...]
        sin = s_ref[...]

        def turned(part, gain):
            x = part.astype(F32)
            a = x * lax.rsqrt(jnp.mean(x * x, axis=-1, keepdims=True) + EPS) * gain
            other = jnp.where(
                low, pltpu.roll(a, width - width // 4, 1), pltpu.roll(a, width // 4, 1)
            )
            return (a * cos + other * sin).astype(BF16)

        for head in range(heads):
            at = (head % per) * width
            o_ref[head // per, :, at : at + width] = turned(
                q_ref[:, head * width : (head + 1) * width], qg_ref[...]
            )
        turned_keys = [
            turned(k_ref[:, h * width : (h + 1) * width], kg_ref[...]) for h in range(kv_heads)
        ]
        for part in range(parts):
            for i in range(kv_per):
                h = (part * per) // group + i
                at = (per + i) * width
                o_ref[part, :, at : at + width] = turned_keys[h]
                at = (per + kv_per + i) * width
                o_ref[part, :, at : at + width] = v_ref[:, h * width : (h + 1) * width]

    return pl.pallas_call(
        body, out_shape=jax.ShapeDtypeStruct((parts, rows, block), BF16), name="pack_rows"
    )(queries, keys, values, query_gain[None], key_gain[None], cosine, sine)


def attend(packed, per, kv_per, width):
    length, full = packed.shape
    rows = min(256, length)

    def body(q_ref, all_ref, o_ref):
        for head in range(per):
            kv = head * kv_per // per
            q = q_ref[:, head * width : (head + 1) * width]
            k = all_ref[:, (per + kv) * width : (per + kv + 1) * width]
            v = all_ref[:, (per + kv_per + kv) * width : (per + kv_per + kv + 1) * width]
            scores = lax.dot_general(
                q, k, (((1,), (1,)), ((), ())), preferred_element_type=F32
            ) * width ** (-0.5)
            e = jnp.exp(scores - jnp.max(scores, axis=-1, keepdims=True))
            weights = (e * (1.0 / jnp.sum(e, axis=-1, keepdims=True))).astype(BF16)
            o_ref[:, head * width : (head + 1) * width] = jnp.dot(
                weights, v, preferred_element_type=F32
            ).astype(BF16)

    return pl.pallas_call(
        body,
        grid=(length // rows,),
        in_specs=[
            pl.BlockSpec((rows, full), lambda i: (i, 0)),
            pl.BlockSpec((length, full), lambda i: (0, 0)),
        ],
        out_specs=pl.BlockSpec((rows, per * width), lambda i: (i, 0)),
        out_shape=jax.ShapeDtypeStruct((length, per * width), BF16),
        name="attend",
    )(packed, packed)


def expert_rows(blocks, gate, up, down):
    count = len(blocks)
    model = blocks[0].shape[1]
    heights = [block.shape[0] for block in blocks]
    starts = [sum(heights[:i]) for i in range(count)]
    total = sum(heights)
    hidden_width = gate.shape[1]
    tile = 256
    steps = hidden_width // tile

    def body(*refs):
        x_refs = refs[:count]
        g_ref, u_ref, d_ref = refs[count : count + 3]
        o_refs = refs[count + 3 : 2 * count + 3]
        x_all, acc = refs[2 * count + 3 :]
        step = pl.program_id(0)

        @pl.when(step == 0)
        def _():
            for i in range(count):
                x_all[starts[i] : starts[i] + heights[i], :] = x_refs[i][...]

        x = x_all[...]
        g = jnp.dot(x, g_ref[...], preferred_element_type=F32)
        u = jnp.dot(x, u_ref[...], preferred_element_type=F32)
        hidden = (g / (1.0 + jnp.exp(-g)) * u).astype(BF16)
        y = jnp.dot(hidden, d_ref[...], preferred_element_type=F32)

        @pl.when(step == 0)
        def _():
            acc[...] = y

        @pl.when(step > 0)
        def _():
            acc[...] += y

        @pl.when(step == steps - 1)
        def _():
            for i in range(count):
                o_refs[i][...] = acc[starts[i] : starts[i] + heights[i], :].astype(BF16)

    whole = [pl.BlockSpec((height, model), lambda i: (0, 0)) for height in heights]
    return pl.pallas_call(
        body,
        grid=(steps,),
        in_specs=whole
        + [
            pl.BlockSpec((model, tile), lambda i: (0, i)),
            pl.BlockSpec((model, tile), lambda i: (0, i)),
            pl.BlockSpec((tile, model), lambda i: (i, 0)),
        ],
        out_specs=whole,
        out_shape=[jax.ShapeDtypeStruct((height, model), BF16) for height in heights],
        scratch_shapes=[
            pltpu.VMEM((total, model), BF16),
            pltpu.VMEM((total, model), F32),
        ],
        name="expert_rows",
    )(*blocks, gate, up, down)


def slots_of(chosen, capacity, experts):
    tokens = chosen.shape[0]
    by_block = chosen.reshape(2, tokens)
    onehot = (by_block[..., None] == jnp.arange(experts, dtype=jnp.int32)).astype(F32)
    earlier = (jnp.arange(tokens)[:, None] > jnp.arange(tokens)[None, :]).astype(F32)
    before = jnp.einsum("ij,bje->bie", earlier, onehot, preferred_element_type=F32)
    rank = jnp.sum(before * onehot, axis=-1).astype(jnp.int32)
    return (jnp.arange(2, dtype=jnp.int32)[:, None] * capacity + rank).reshape(tokens, 2)


def on_device(
    queries, key_rows, values, query_gain, key_gain, out_weight, residual, norm_gain,
    expert_gate, expert_up, expert_down, routes, route_weight,
):
    parts = lax.axis_size("sp")
    columns = lax.axis_size("dp")
    me = lax.axis_index("sp")
    _, tokens, heads, width = queries.shape
    kv_heads = key_rows.shape[2]
    group = heads // kv_heads
    per = heads // parts
    kv_per = max(1, per // group)
    half = parts // 2
    near = parts // 4

    positions = me * tokens + jnp.arange(tokens, dtype=jnp.int32)
    cosine, sine = angle_tables(positions, width)
    packed = pack_rows(
        queries.reshape(tokens, heads * width),
        key_rows.reshape(tokens, kv_heads * width),
        values.reshape(tokens, kv_heads * width),
        query_gain, key_gain, cosine, sine, parts,
    )
    by_head = lax.all_to_all(packed, "sp", split_axis=0, concat_axis=0, tiled=True)

    shards = [None] * 4
    for far in range(4):
        shards[far] = out_weight if far == 0 else swap(out_weight, "sp", far * near)

    experts = expert_gate.shape[0] * parts
    capacity = max(2, 4 * (tokens // 2) // experts)
    slots = 2 * capacity
    chosen = routes[0]
    slot = slots_of(chosen, capacity, experts)
    weight = route_weight[0]
    chosen_far = swap(chosen, "sp", half)
    slot_far = swap(slot, "sp", half)
    weight_far = swap(weight, "sp", half)

    def selection(chosen, slot, first, count):
        place = jnp.arange(half * count, dtype=jnp.int32)
        expert = me ^ (place // count)
        place_slot = first + place % count
        return [
            (chosen[:, j, None] == expert[None]) & (slot[:, j, None] == place_slot[None])
            for j in range(2)
        ]

    block = tokens // 2
    spans = [slice(b * block, (b + 1) * block) for b in range(2)]
    pick = selection(chosen, slot, 0, slots)
    picks_far = [
        selection(chosen_far[spans[b]], slot_far[spans[b]], b * capacity, capacity)
        for b in range(2)
    ]

    attended = attend(by_head.reshape(parts * tokens, -1), per, kv_per, width)
    attended, shards = lax.optimization_barrier((attended, shards))
    whole = []
    for far in range(4):
        whole.append(shards[far])
        for close in range(1, near):
            whole.append(swap(shards[far], "sp", close))
    returned = lax.all_to_all(
        attended.reshape(parts, tokens, per * width), "sp", split_axis=0, concat_axis=0, tiled=True
    )
    rows = jnp.concatenate(
        [lax.dynamic_index_in_dim(returned, me ^ k, 0, keepdims=False) for k in range(parts)],
        axis=1,
    )

    chips = columns // 2
    peers = []
    for k in range(1, chips):
        peers.append(swap(rows, "dp", 2 * k))
    _, whole = lax.optimization_barrier((rows, whole))
    own_columns = jnp.concatenate(whole, axis=0)
    core_columns = swap(own_columns, "dp", 1)
    gathered = jnp.concatenate([rows] + peers, axis=0)
    mine = jnp.dot(gathered, own_columns, preferred_element_type=F32).astype(BF16)
    other = jnp.dot(gathered, core_columns, preferred_element_type=F32).astype(BF16)
    first = lax.axis_index("dp") % 2 == 0
    both = jnp.concatenate(
        [jnp.where(first, mine, other), jnp.where(first, other, mine)], axis=1
    ).reshape(chips, tokens, -1)
    back = [both[0]] + [swap(both[k], "dp", 2 * k) for k in range(1, chips)]
    chip = lax.axis_index("dp") // 2
    if chips == 2:
        ordered = [jnp.where(chip == 0, back[0], back[1]), jnp.where(chip == 0, back[1], back[0])]
    else:
        stacked = jnp.stack(back)
        ordered = [
            lax.dynamic_index_in_dim(stacked, chip ^ k, 0, keepdims=False) for k in range(chips)
        ]
    projected = jnp.concatenate(ordered, axis=1).astype(F32)
    mixed_sum = residual[0].astype(F32) + projected
    normed = (
        mixed_sum
        * lax.rsqrt(jnp.mean(mixed_sum * mixed_sum, axis=-1, keepdims=True) + EPS)
        * norm_gain
    ).astype(BF16)

    crossed = [swap(normed[span], "sp", half) for span in spans]

    def send(source, picks, count):
        chosen_rows = (picks[0] | picks[1]).astype(BF16)
        sent = lax.dot_general(
            chosen_rows, source, (((0,), (0,)), ((), ())), preferred_element_type=F32
        ).astype(BF16)
        return exchange([sent[k * count : (k + 1) * count] for k in range(half)])

    def exchange(blocks):
        return [blocks[0]] + [swap(blocks[k], "sp", k) for k in range(1, half)]

    def combine(results, picks, weight):
        flat = jnp.concatenate(results, axis=0)
        return sum(
            jnp.dot(picks[j].astype(BF16), flat, preferred_element_type=F32) * weight[:, j, None]
            for j in range(2)
        )

    sent = send(normed, pick, slots)
    for b in range(2):
        sent = sent + send(crossed[b], picks_far[b], capacity)
    results = expert_rows(sent, expert_gate[0], expert_up[0], expert_down[0])
    back = []
    for b in range(2):
        far_results = exchange(results[(b + 1) * half : (b + 2) * half])
        part = combine(far_results, picks_far[b], weight_far[spans[b]]).astype(BF16)
        back.append(swap(part, "sp", half))
    near_results = exchange(results[:half])
    near_part = combine(near_results, pick, weight)
    result = mixed_sum + near_part + jnp.concatenate(back, axis=0).astype(F32)
    return result.astype(BF16)[None]


def solution(mesh):
    in_specs = (
        P("dp", "sp", None, None),
        P("dp", "sp", None, None),
        P("dp", "sp", None, None),
        P(),
        P(),
        P("sp", "dp"),
        P("dp", "sp", None),
        P(),
        P("sp", None, None),
        P("sp", None, None),
        P("sp", None, None),
        P("dp", "sp", None),
        P("dp", "sp", None),
    )
    out_specs = P("dp", "sp", None)

    return jax.shard_map(
        on_device, mesh=mesh, in_specs=in_specs, out_specs=out_specs, check_vma=False
    )
```
